32 devices in a mesh: sp: 8 (over z, x), tp: 4 (over y, core).
Axes of the slice: x: 2, y: 2, z: 4, core: 2. Of those that a mesh axis runs over, the one named last changes fastest.
Arguments:
- queries: bfloat16 [512, 1024], P('tp', 'sp'), may hold values from -6 to 6
- input_key_matrix: bfloat16 [512, 1024], P('tp', 'sp'), may hold values from -6 to 6
- input_value_matrix: bfloat16 [1024, 1024], P('tp', 'sp'), may hold values from -6 to 6
- decay_preactivation: bfloat16 [512, 1024], P('tp', 'sp'), may hold values from -6 to 6
- extra_log_decay: float32 [512, 1024], P('tp', 'sp'), may hold values from -1 to 0, as said below
- channel_decay_speed: float32 [512], P('tp'), may hold values from 0 to 1, as said below
- output_weight_matrix: bfloat16 [2048, 1024], P(None, 'tp'), may hold values from -0.1875 to 0.1875
- stored_expert_rows: bfloat16 [1024, 2048], P('sp', 'tp'), may hold values from -6 to 6
- chosen_expert_index: int32 [1024, 2], P('sp'), may hold values from 0 to 7, all different within a row; in each aligned block of 128 rows (0 to 127, 128 to 255, ...) at most 48 rows name the same one
- expert_combine_weight: float32 [1024, 2], P('sp'), may hold values from 0.2 to 1
- cotangent: bfloat16 [1024, 2048], P('sp', 'tp'), may hold values from -6 to 6
- expert_gate_weight: bfloat16 [8, 2048, 2048], P('sp', None, 'tp'), may hold values from -0.125 to 0.125
- expert_up_weight: bfloat16 [8, 2048, 2048], P('sp', None, 'tp'), may hold values from -0.125 to 0.125
- expert_down_weight: bfloat16 [8, 2048, 2048], P('sp', 'tp'), may hold values from -0.125 to 0.125
Outputs:
- grad_queries: float32 [512, 1024], P('tp', 'sp')
- grad_keys: float32 [512, 1024], P('tp', 'sp')
- grad_values: float32 [1024, 1024], P('tp', 'sp')
- grad_logit: float32 [512, 1024], P('tp', 'sp')
- grad_out_proj: float32 [2048, 1024], P('sp', 'tp')
- grad_gate: bfloat16 [8, 2048, 2048], P('sp', None, 'tp')
- grad_up: bfloat16 [8, 2048, 2048], P('sp', None, 'tp')
- grad_down: bfloat16 [8, 2048, 2048], P('sp', 'tp')
The draws below stay inside these ranges and needn't reach their ends.
Inputs may be any that keep to these rules, and one draw needn't show every extreme that they name: `chosen_expert_index`: each position names two different experts; in the rows of one device no expert is named more than 48 times. `channel_decay_speed`: positive. `extra_log_decay`: zero or negative.
All inputs are finite; a program needn't handle non-finite values.
Results may differ from the reference program's by a relative error of at most 0.023.
Values may be sent and summed in bfloat16 or wider, within the bound.
A program may use at most 64 MiB of HBM per device.

```python
import math
import jax
import jax.numpy as jnp
import numpy as np
from jax import lax

D = 2048
HEADS = 16
KEY_DIM = 32
VAL_DIM = 64
EXPERT_UNITS = 2048
TOK_DEV = 128
SPAN = 64
SEQUENCE_LENGTH = 1024
EXPERTS = 8
CAP = 48
KEY_CHANNELS = 512
VCH = 1024
N_SP = 8
N_TP = 4


def draw_channel_decay_speed(key, part):
    key_pick, key_spread = jax.random.split(jax.random.fold_in(key, 11))
    slow_share = 0.5
    is_slow = jax.random.uniform(key_pick, (KEY_CHANNELS,), jnp.float32) < slow_share
    spread = jax.random.uniform(key_spread, (KEY_CHANNELS,), jnp.float32)
    slow_rate = jnp.exp(jnp.log(0.2) + spread * (jnp.log(1.0) - jnp.log(0.2))) / SEQUENCE_LENGTH
    fast_rate = jnp.exp(jnp.log(0.02) + spread * (jnp.log(0.06) - jnp.log(0.02)))
    return jnp.where(is_slow, slow_rate, fast_rate).astype(jnp.float32)


def draw_decay_preactivation(key, part):
    key_noise, key_level = jax.random.split(jax.random.fold_in(key, 23))
    noise = jnp.clip(jax.random.normal(key_noise, (KEY_CHANNELS, SEQUENCE_LENGTH), jnp.float32), -4.0, 4.0)
    level = jax.random.uniform(key_level, (SEQUENCE_LENGTH // TOK_DEV,), jnp.float32, -1.5, 1.5)
    return (noise + jnp.repeat(level, TOK_DEV)[None, :]).astype(jnp.bfloat16)


def draw_extra_log_decay(key, part):
    key_channel_index, key_channel_count = jax.random.split(jax.random.fold_in(key, 37))
    jump_location = jax.random.randint(key_channel_index, (KEY_CHANNELS, 3), 0, SEQUENCE_LENGTH)
    jump_magnitude = jax.random.uniform(key_channel_count, (KEY_CHANNELS, 3), jnp.float32, jnp.log(0.6), jnp.log(0.8))
    jump_hit_mask = jnp.arange(SEQUENCE_LENGTH, dtype=jnp.int32)[None, None, :] == jump_location[:, :, None]
    return jnp.sum(jnp.where(jump_hit_mask, jump_magnitude[:, :, None], 0.0), axis=1).astype(jnp.float32)


def raised(values, key, source, target, shards_of, factor):
    def block_of(axis_at):
        return (jnp.arange(values.shape[axis_at]) // (values.shape[axis_at] // shards_of)).reshape((-1,) + (1,) * (values.ndim - 1 - axis_at))

    one_side = jax.random.permutation(key, shards_of)[block_of(target)]
    second = (block_of(target) + shards_of // 2) % shards_of
    return jnp.where((block_of(source) == one_side) | (block_of(source) == second), factor * values, values)


def levels(key, dims, cuts, smallest, top_value):
    level = 1.0
    for axis_at, shards_of in cuts:
        draws = jax.random.uniform(jax.random.fold_in(jax.random.fold_in(key, 6), axis_at), (shards_of,), jnp.float32, smallest / len(cuts), top_value / len(cuts))
        level = level * jnp.repeat(jnp.exp(draws), dims[axis_at] // shards_of).reshape((-1,) + (1,) * (len(dims) - 1 - axis_at))
    return level


def assign_block(key, own, number, rows, number_of, top, most, slope):
    order = jax.random.permutation(key, number_of)
    crowded, ordinary = load_shares(number_of, rows * top, most, slope, True), load_shares(number_of, rows * top, most, slope, False)
    places = jnp.arange(number_of)

    def named(sizes, offset_by):
        used = int((sizes > 0).sum())
        fixed = max(1, used // 4)
        moved = fixed + (places - fixed + offset_by * (used - fixed)) % max(1, number_of - fixed)
        return jnp.zeros((number_of,), jnp.int32).at[order[jnp.where(places < fixed, places, moved)]].set(jnp.asarray(sizes, jnp.int32))

    sizes = jnp.where(number % 4 == 0, named(crowded, number // 4), named(ordinary, number - number // 4 - 1))
    mixed = jax.random.permutation(jax.random.fold_in(own, 3), number_of)
    donor, receiver = mixed[0:number_of // 2 * 2:2], mixed[1:number_of // 2 * 2:2]
    margin = jnp.minimum(sizes[donor] - 1, most - sizes[receiver]) // 2
    margin = jnp.where((donor == order[0]) | (receiver == order[0]) | (sizes[receiver] == 0), 0, jnp.maximum(margin, 0))
    moved = jax.random.randint(jax.random.fold_in(own, 4), (number_of // 2,), 0, 1 << 20) % (margin + 1)
    sizes = sizes.at[donor].add(-moved).at[receiver].add(moved)
    items = jnp.searchsorted(jnp.cumsum(sizes), jnp.arange(rows * top), side="right").astype(jnp.int32)
    table = items.reshape(top, rows).T
    table = table[jax.random.permutation(jax.random.fold_in(own, 1), rows)]
    offset_by = jax.random.randint(jax.random.fold_in(own, 2), (rows, 1), 0, top)
    return jnp.take_along_axis(table, (jnp.arange(top)[None, :] + offset_by) % top, axis=1)


def load_shares(count, total, bound, lean, full):
    portions = [(1 << 20) // math.isqrt(rank ** lean) + 1 for rank in range(1, count + 1)]
    largest = bound if full else min(bound, max(-(-total // count), total * portions[0] // sum(portions)))
    least = 1 if total - largest >= count - 1 else 0
    holding, rest = [largest] + [least] * (count - 1), total - largest - least * (count - 1)
    while rest > 0:
        free = [i for i in range(1, count) if holding[i] < largest] or [i for i in range(1, count) if holding[i] < bound]
        mass, left = sum([portions[i] for i in free]), rest
        for i in free:
            extra = min(bound - holding[i], max(1, left * portions[i] // mass), rest)
            holding[i] = holding[i] + extra
            rest = rest - extra
    return np.array(holding)


def normal_values(rng, shape, deviation, limit, shards=(), kind=jnp.bfloat16):
    factor_of = levels(rng, shape, shards, -0.22, 0.18) if shards else 1.0
    drawn = jax.random.normal(rng, shape, jnp.float32) * deviation * factor_of
    return jnp.minimum(jnp.maximum(drawn, -limit), limit).astype(kind)


def bell_draw_with(rng, extent, width, bound, cuts, heavy, kind=jnp.bfloat16):
    entries = width * jax.random.normal(rng, extent, jnp.float32)
    if cuts:
        entries = entries * levels(rng, extent, cuts, -0.22, 0.18)
    return jnp.clip(raised(entries, jax.random.fold_in(rng, 3), *heavy), -bound, bound).astype(kind)


def setup_inputs(seed: int = 0) -> dict:
    keys = jax.random.split(jax.random.key(seed), 15)
    queries = normal_values(keys[0], (KEY_CHANNELS, SEQUENCE_LENGTH), 1.0, 6.0, ((0, 4), (1, 8)))
    input_key_matrix = normal_values(keys[1], (KEY_CHANNELS, SEQUENCE_LENGTH), 1.0, 6.0, ((0, 4), (1, 8)))
    input_value_matrix = normal_values(keys[2], (VCH, SEQUENCE_LENGTH), 1.0, 6.0, ((0, 4), (1, 8)))
    decay_preactivation = draw_decay_preactivation(jax.random.fold_in(keys[14], 71), 0)
    extra_log_decay = draw_extra_log_decay(jax.random.fold_in(keys[14], 71), 0)
    channel_decay_speed = draw_channel_decay_speed(jax.random.fold_in(keys[14], 71), 0)
    output_weight_matrix = normal_values(keys[6], (D, VCH), VCH ** -0.5, 0.1875, ((1, 4),))
    stored_expert_rows = normal_values(keys[7], (SEQUENCE_LENGTH, D), 1.0, 6.0, ((0, 8), (1, 4)))
    chosen_expert_index_keys = jax.random.split(jax.random.fold_in(keys[8], 1), SEQUENCE_LENGTH // TOK_DEV)
    chosen_expert_index_turns = jax.random.permutation(jax.random.fold_in(keys[8], 3), SEQUENCE_LENGTH // TOK_DEV)
    chosen_expert_index = jax.vmap(lambda own, number: assign_block(jax.random.fold_in(keys[8], 2), own, number, TOK_DEV, EXPERTS, 2, CAP, 1))(chosen_expert_index_keys, chosen_expert_index_turns).reshape((SEQUENCE_LENGTH, 2))
    expert_combine_weight = jnp.clip(0.2 + 0.8 * jax.random.uniform(keys[9], (SEQUENCE_LENGTH, 2), jnp.float32) ** levels(keys[9], (SEQUENCE_LENGTH, 2), ((0, 8),), -0.2, 0.2), 0.2, 1.0)
    cotangent = bell_draw_with(keys[10], (SEQUENCE_LENGTH, D), 1.0, 6.0, ((0, 8), (1, 4)), (0, 1, 8, 2.0))
    expert_gate_weight = normal_values(keys[11], (EXPERTS, D, EXPERT_UNITS), D ** -0.5, 0.125, ((0, 8), (2, 4)))
    expert_up_weight = normal_values(keys[12], (EXPERTS, D, EXPERT_UNITS), D ** -0.5, 0.125, ((0, 8), (2, 4)))
    expert_down_weight = normal_values(keys[13], (EXPERTS, EXPERT_UNITS, D), EXPERT_UNITS ** -0.5, 0.125, ((0, 8), (1, 4)))
    return dict(queries=queries, input_key_matrix=input_key_matrix, input_value_matrix=input_value_matrix, decay_preactivation=decay_preactivation, extra_log_decay=extra_log_decay, channel_decay_speed=channel_decay_speed, output_weight_matrix=output_weight_matrix, stored_expert_rows=stored_expert_rows, chosen_expert_index=chosen_expert_index, expert_combine_weight=expert_combine_weight, cotangent=cotangent, expert_gate_weight=expert_gate_weight, expert_up_weight=expert_up_weight, expert_down_weight=expert_down_weight)


def combine_steps(state, pair):
    factor, addend = pair
    return (factor * state + addend, state)

def head_forward(scaled, key_feats, val_feats, decay_logarithm):
    blocks = decay_logarithm.shape[1] // SPAN

    def split_blocks(array):
        return array.reshape(array.shape[0], blocks, SPAN).transpose(1, 0, 2)
    block_q = split_blocks(scaled)
    block_k = split_blocks(key_feats)
    block_v = split_blocks(val_feats)
    cumulative = jnp.cumsum(split_blocks(decay_logarithm), axis=2)
    total_log = cumulative[:, :, -1:]
    lower_mask = lax.broadcasted_iota(jnp.int32, (SPAN, SPAN), 0) >= lax.broadcasted_iota(jnp.int32, (SPAN, SPAN), 1)
    log_gap = cumulative[:, :, :, None] - cumulative[:, :, None, :]
    weight = jnp.exp(jnp.where(lower_mask, log_gap, -log_gap))
    scores = jnp.einsum('bct,bcs,bcts->bts', block_q, block_k, weight)
    inner_part = jnp.einsum('bts,bvs->bvt', scores, block_v)
    factor = jnp.exp(total_log)
    fwd_sum = jnp.einsum('bcs,bvs->bcv', block_k * jnp.exp(total_log - cumulative), block_v)
    bwd_sum = jnp.einsum('bcs,bvs->bcv', block_k * jnp.exp(cumulative), block_v)
    start_state = jnp.zeros((key_feats.shape[0], val_feats.shape[0]), jnp.float32)
    _, fwd_in = lax.scan(combine_steps, start_state, (factor, fwd_sum))
    _, bwd_in = lax.scan(combine_steps, start_state, (factor, bwd_sum), reverse=True)
    carried = jnp.einsum('bct,bcv->bvt', block_q * jnp.exp(cumulative), fwd_in)
    carried = carried + jnp.einsum('bct,bcv->bvt', block_q * jnp.exp(total_log - cumulative), bwd_in)
    output = inner_part + carried
    return output.transpose(1, 0, 2).reshape(val_feats.shape[0], -1)

def head_mix(query_f, key_feats, val_feats, decay_logarithm):
    return head_forward(query_f * KEY_DIM ** (-0.5), key_feats, val_feats, decay_logarithm)

def head_apply(packed):
    return head_mix(packed[0], packed[1], packed[2], packed[3])

def head_grads(packed):
    _, pull_back = jax.vjp(head_mix, packed[0], packed[1], packed[2], packed[3])
    return pull_back(packed[4])

def expert_grads(packed):
    slot_table, gate_local, up_local, down_local, inputs_pad, grads_pad = packed
    rows_x = inputs_pad[slot_table // 2]
    rows_dy = grads_pad[slot_table]
    gate_pre = jnp.dot(rows_x, gate_local, preferred_element_type=jnp.float32)
    up_pre = jnp.dot(rows_x, up_local, preferred_element_type=jnp.float32)
    gate_sig = jax.nn.sigmoid(gate_pre)
    gate_act = gate_pre * gate_sig
    hidden = (gate_act * up_pre).astype(jnp.bfloat16)
    grad_down = jnp.dot(hidden.T, rows_dy, preferred_element_type=jnp.float32).astype(jnp.bfloat16)
    grad_hidden = jnp.dot(rows_dy, down_local.T, preferred_element_type=jnp.float32)
    grad_gate_pre = (grad_hidden * up_pre * gate_sig * (1.0 + gate_pre * (1.0 - gate_sig))).astype(jnp.bfloat16)
    grad_up_pre = (grad_hidden * gate_act).astype(jnp.bfloat16)
    grad_gate = jnp.dot(rows_x.T, grad_gate_pre, preferred_element_type=jnp.float32).astype(jnp.bfloat16)
    grad_up = jnp.dot(rows_x.T, grad_up_pre, preferred_element_type=jnp.float32).astype(jnp.bfloat16)
    row_count = rows_x.shape[0]
    group_width = EXPERT_UNITS // N_TP
    gate_groups = grad_gate_pre.astype(jnp.float32).reshape(row_count, N_TP, group_width)
    up_groups = grad_up_pre.astype(jnp.float32).reshape(row_count, N_TP, group_width)
    gate_weights = gate_local.astype(jnp.float32).reshape(D, N_TP, group_width)
    up_weights = up_local.astype(jnp.float32).reshape(D, N_TP, group_width)
    partial_value = jnp.einsum('rjh,djh->jrd', gate_groups, gate_weights) + jnp.einsum('rjh,djh->jrd', up_groups, up_weights)
    partial_value = partial_value.astype(jnp.bfloat16).astype(jnp.float32)
    slot_grads = lax.optimization_barrier(jnp.sum(partial_value, axis=0)).astype(jnp.bfloat16)
    return (grad_gate, grad_up, grad_down, slot_grads)

def reference(queries, input_key_matrix, input_value_matrix, decay_preactivation, extra_log_decay, channel_decay_speed, output_weight_matrix, stored_expert_rows, chosen_expert_index, expert_combine_weight, cotangent, expert_gate_weight, expert_up_weight, expert_down_weight):
    preactivation_single = decay_preactivation.astype(jnp.float32)
    decay_logarithm = channel_decay_speed[:, None] * jax.nn.log_sigmoid(preactivation_single) + extra_log_decay
    query_heads = queries.astype(jnp.float32).reshape(HEADS, KEY_DIM, SEQUENCE_LENGTH)
    key_heads = input_key_matrix.astype(jnp.float32).reshape(HEADS, KEY_DIM, SEQUENCE_LENGTH)
    value_heads = input_value_matrix.astype(jnp.float32).reshape(HEADS, VAL_DIM, SEQUENCE_LENGTH)
    decay_heads = decay_logarithm.reshape(HEADS, KEY_DIM, SEQUENCE_LENGTH)
    mixed = lax.map(head_apply, (query_heads, key_heads, value_heads, decay_heads))
    inv_rms = lax.rsqrt(lax.optimization_barrier(jnp.mean(mixed * mixed, axis=1, keepdims=True)) + 1e-06)
    normed = mixed * inv_rms
    mix_rows = normed.astype(jnp.bfloat16).reshape(VCH, SEQUENCE_LENGTH)
    block_ids = chosen_expert_index.reshape(N_SP, 2 * TOK_DEV)
    onehot = (block_ids[:, :, None] == jnp.arange(EXPERTS, dtype=jnp.int32)[None, None, :]).astype(jnp.int32)
    slot_rank = lax.optimization_barrier(jnp.sum((jnp.cumsum(onehot, axis=1) - onehot) * onehot, axis=2))
    source = jnp.arange(N_SP, dtype=jnp.int32)[:, None]
    flat_slot = (block_ids * (N_SP * CAP) + source * CAP + slot_rank).reshape(-1)
    slot_table = jnp.full((EXPERTS * N_SP * CAP,), 2 * SEQUENCE_LENGTH, jnp.int32)
    slot_table = slot_table.at[flat_slot].set(jnp.arange(2 * SEQUENCE_LENGTH, dtype=jnp.int32))
    zero_row = jnp.zeros((1, D), jnp.bfloat16)
    inputs_pad = jnp.concatenate([stored_expert_rows, zero_row], axis=0)
    weighted = (expert_combine_weight.reshape(-1, 1) * jnp.repeat(cotangent, 2, axis=0).astype(jnp.float32)).astype(jnp.bfloat16)
    grads_pad = jnp.concatenate([weighted, zero_row], axis=0)

    def per_expert(packed):
        return expert_grads((packed[0], packed[1], packed[2], packed[3], inputs_pad, grads_pad))
    grad_gate, grad_up, grad_down, slot_grads = lax.map(per_expert, (slot_table.reshape(EXPERTS, N_SP * CAP), expert_gate_weight, expert_up_weight, expert_down_weight))
    picked = slot_grads.reshape(EXPERTS * N_SP * CAP, D)[flat_slot].astype(jnp.float32).reshape(SEQUENCE_LENGTH, 2, D)
    token_grads = (cotangent.astype(jnp.float32) + picked[:, 0] + picked[:, 1]).astype(jnp.bfloat16)
    grad_out_proj = jnp.dot(token_grads.T, mix_rows.T, preferred_element_type=jnp.float32)
    grad_normed = jnp.dot(output_weight_matrix.T, token_grads.T, preferred_element_type=jnp.float32).reshape(HEADS, VAL_DIM, SEQUENCE_LENGTH)
    grad_mixed = inv_rms * (grad_normed - normed * lax.optimization_barrier(jnp.mean(grad_normed * normed, axis=1, keepdims=True)))
    grad_q, grad_k, grad_v, grad_decay = lax.map(head_grads, (query_heads, key_heads, value_heads, decay_heads, grad_mixed))
    grad_logit = grad_decay.reshape(KEY_CHANNELS, SEQUENCE_LENGTH) * channel_decay_speed[:, None] * jax.nn.sigmoid(-preactivation_single)
    return (grad_q.reshape(KEY_CHANNELS, SEQUENCE_LENGTH), grad_k.reshape(KEY_CHANNELS, SEQUENCE_LENGTH), grad_v.reshape(VCH, SEQUENCE_LENGTH), grad_logit, grad_out_proj, grad_gate, grad_up, grad_down)
```

```python
import functools

import jax
import jax.numpy as jnp
from jax import lax
from jax.experimental import pallas as pl
from jax.experimental.pallas import tpu as pltpu
from jax.sharding import PartitionSpec as P

KEY_DIM = 32
VAL_DIM = 64
BF16 = jnp.bfloat16
F32 = jnp.float32


def dot(a, b, contract):
    return lax.dot_general(a.astype(BF16), b.astype(BF16), (contract, ((), ())),
                           preferred_element_type=F32)


def exact_dot(a, b):
    return lax.dot_general(a, b, (((1,), (0,)), ((), ())), precision=lax.Precision.HIGHEST,
                           preferred_element_type=F32)


def triangle(length, test):
    rows = lax.broadcasted_iota(jnp.int32, (length, length), 0)
    cols = lax.broadcasted_iota(jnp.int32, (length, length), 1)
    return test(rows, cols)


def head_kernel(q_ref, k_ref, v_ref, pre_ref, extra_ref, speed_ref,
                st_ref, inner_ref, cum_ref, fwd_ref, bwd_ref):
    length = q_ref.shape[1]
    q = q_ref[...].astype(F32) * KEY_DIM ** (-0.5)
    k = k_ref[...].astype(F32)
    v = v_ref[...]
    pre = pre_ref[...].astype(F32)
    log_sig = jnp.minimum(pre, 0.0) - jnp.log1p(jnp.exp(-jnp.abs(pre)))
    decays = speed_ref[...] * log_sig + extra_ref[...]
    upto = triangle(length, lambda a, b: a <= b).astype(F32)
    cum = exact_dot(decays, upto)
    cum_ref[...] = cum
    cum_t = cum.T
    k_t = k.T
    total = jnp.zeros((length, length), F32)
    for c in range(KEY_DIM):
        weight = jnp.exp(-jnp.abs(cum_t[:, c:c + 1] - cum[c:c + 1, :]))
        total = total + (k_t[:, c:c + 1] * q[c:c + 1, :]) * weight
    scores = total.astype(BF16)
    st_ref[...] = scores
    inner_ref[...] = dot(v, scores, ((1,), (0,)))
    last = cum[:, length - 1:length]
    fwd = dot(k * jnp.exp(last - cum), v, ((1,), (1,)))
    bwd = dot(k * jnp.exp(cum), v, ((1,), (1,)))
    high = last.astype(BF16)
    rest = last - high.astype(F32)
    middle = rest.astype(BF16)
    low = (rest - middle.astype(F32)).astype(BF16)
    lane = lax.broadcasted_iota(jnp.int32, (KEY_DIM, VAL_DIM), 1)
    logs = jnp.where(lane == 0, high.astype(F32),
                     jnp.where(lane == 1, middle.astype(F32), low.astype(F32)))
    fwd_ref[...] = jnp.concatenate([fwd, logs], axis=1).astype(BF16)
    bwd_ref[...] = jnp.concatenate([bwd, logs], axis=1).astype(BF16)


def carry(recv, me, sums_of, factors):
    peers = recv.shape[0]
    zero = jnp.zeros((KEY_DIM, VAL_DIM), F32)
    before, after = zero, zero
    for i in range(peers):
        before = jnp.where(i < me, before * factors[i] + sums_of(i), before)
    for i in reversed(range(peers)):
        after = jnp.where(i > me, after * factors[i] + sums_of(i), after)
    return before, after


def factors_of(recv):
    out = []
    for i in range(recv.shape[0]):
        logs = recv[i, :, VAL_DIM:VAL_DIM + 3].astype(F32)
        out.append(jnp.exp(logs[:, 0:1] + logs[:, 1:2] + logs[:, 2:3]))
    return out


def mix_kernel(me_ref, recv_ref, q_ref, cum_ref, inner_ref,
               carried_ref, normed_ref, inv_ref, rows_ref):
    length = q_ref.shape[1]
    me = me_ref[0]
    fwd_in, bwd_in = carry(
        recv_ref, me, lambda i: recv_ref[i, :, :VAL_DIM].astype(F32), factors_of(recv_ref))
    carried_ref[...] = jnp.concatenate([fwd_in, bwd_in], axis=1)
    q = q_ref[...].astype(F32) * KEY_DIM ** (-0.5)
    cum = cum_ref[...]
    last = cum[:, length - 1:length]
    mixed = inner_ref[...] + dot(fwd_in, q * jnp.exp(cum), ((0,), (0,)))
    mixed = mixed + dot(bwd_in, q * jnp.exp(last - cum), ((0,), (0,)))
    inv = lax.rsqrt(jnp.mean(mixed * mixed, axis=0, keepdims=True) + 1e-06)
    normed = mixed * inv
    normed_ref[...] = normed
    inv_ref[...] = jnp.broadcast_to(inv, inv_ref.shape)
    rows_ref[...] = normed.astype(BF16)


def source_kernel(gn_ref, normed_ref, inv_ref, q_ref, cum_ref, dm_ref, fwd_ref, bwd_ref):
    length = q_ref.shape[1]
    normed = normed_ref[...]
    gn = gn_ref[...]
    dm = inv_ref[0:1, :] * (gn - normed * jnp.mean(gn * normed, axis=0, keepdims=True))
    dm_ref[...] = dm
    q = q_ref[...].astype(F32) * KEY_DIM ** (-0.5)
    cum = cum_ref[...]
    last = cum[:, length - 1:length]
    fwd = dot(q * jnp.exp(cum), dm, ((1,), (1,)))
    bwd = dot(q * jnp.exp(last - cum), dm, ((1,), (1,)))
    pad = jnp.zeros_like(fwd)
    fwd_ref[...] = jnp.concatenate([fwd, pad], axis=1).astype(BF16)
    bwd_ref[...] = jnp.concatenate([bwd, pad], axis=1).astype(BF16)


def inner_kernel(dm_ref, q_ref, k_ref, v_ref, cum_ref, st_ref, carried_ref,
                 dq_ref, dk_ref, dv_ref, dc_ref, dt_ref):
    length = q_ref.shape[1]
    dm = dm_ref[...]
    q = q_ref[...].astype(F32) * KEY_DIM ** (-0.5)
    k = k_ref[...].astype(F32)
    v = v_ref[...]
    cum = cum_ref[...]
    by_query = dot(dm, v, ((0,), (0,)))
    by_key = dot(v, dm, ((0,), (0,)))
    sign = jnp.where(triangle(length, lambda a, b: a > b), 1.0,
                     jnp.where(triangle(length, lambda a, b: a < b), -1.0, 0.0)).astype(F32)
    by_query_signed = by_query * sign
    by_key_signed = by_key * -sign
    cum_t, q_t, k_t = cum.T, q.T, k.T
    dq, dk, dq_signed, dk_signed = [], [], [], []
    for c in range(KEY_DIM):
        weight = jnp.exp(-jnp.abs(cum_t[:, c:c + 1] - cum[c:c + 1, :]))
        with_q = weight * q_t[:, c:c + 1]
        with_k = weight * k_t[:, c:c + 1]
        dk.append(jnp.sum(by_query * with_q, axis=0, keepdims=True))
        dk_signed.append(jnp.sum(by_query_signed * with_q, axis=0, keepdims=True))
        dq.append(jnp.sum(by_key * with_k, axis=0, keepdims=True))
        dq_signed.append(jnp.sum(by_key_signed * with_k, axis=0, keepdims=True))
    join = lambda rows: jnp.concatenate(rows, axis=0)
    last = cum[:, length - 1:length]
    carried = carried_ref[...]
    up, down = jnp.exp(cum), jnp.exp(last - cum)
    d_up = dot(carried[:, :VAL_DIM], dm, ((1,), (0,))) * up
    d_down = dot(carried[:, VAL_DIM:], dm, ((1,), (0,))) * down
    dq_ref[...] = (join(dq) + d_up + d_down) * KEY_DIM ** (-0.5)
    dk_ref[...] = join(dk)
    dv_ref[...] = dot(dm, st_ref[...], ((1,), (1,)))
    dc_ref[...] = q * (join(dq_signed) + d_up - d_down) - k * join(dk_signed)
    dt_ref[...] = jnp.broadcast_to(
        jnp.sum(q * d_down, axis=1, keepdims=True), dt_ref.shape)


def last_kernel(me_ref, recv_ref, first_ref, carried_ref, k_ref, v_ref, cum_ref,
                pre_ref, speed_ref, dk_in_ref, dv_in_ref, dc_in_ref, dt_ref,
                dk_ref, dv_ref, logit_ref):
    length = k_ref.shape[1]
    me = me_ref[0]
    grad_bwd, grad_fwd = carry(
        recv_ref, me, lambda i: recv_ref[i, :, :VAL_DIM].astype(F32), factors_of(first_ref))
    k = k_ref[...].astype(F32)
    v = v_ref[...]
    cum = cum_ref[...]
    last = cum[:, length - 1:length]
    up, down = jnp.exp(cum), jnp.exp(last - cum)
    d_down = dot(grad_fwd, v, ((1,), (0,))) * down
    d_up = dot(grad_bwd, v, ((1,), (0,))) * up
    dk_ref[...] = dk_in_ref[...] + d_down + d_up
    dv_ref[...] = (dv_in_ref[...] + dot(grad_fwd, k * down, ((0,), (0,)))
                   + dot(grad_bwd, k * up, ((0,), (0,))))
    carried = carried_ref[...]
    grad_factor = jnp.sum(grad_fwd * carried[:, :VAL_DIM] + grad_bwd * carried[:, VAL_DIM:],
                          axis=1, keepdims=True)
    grad_total = (dt_ref[:, 0:1] + jnp.sum(k * d_down, axis=1, keepdims=True)
                  + grad_factor * jnp.exp(last))
    dc = dc_in_ref[...] + k * (d_up - d_down)
    from_here = triangle(length, lambda a, b: a >= b).astype(F32)
    grad_decay = exact_dot(dc, from_here) + grad_total
    pre = pre_ref[...].astype(F32)
    logit_ref[...] = grad_decay * speed_ref[...] * jax.nn.sigmoid(-pre)


def per_head(kernel, heads, outs, args, vmem_ops, scalars=0):
    def spec(shape):
        if len(shape) == 3:
            return pl.BlockSpec((shape[0], shape[1] // heads, shape[2]), lambda h: (0, h, 0))
        return pl.BlockSpec((shape[0] // heads, shape[1]), lambda h: (h, 0))

    in_specs = [pl.BlockSpec(memory_space=pltpu.SMEM)] * scalars
    in_specs += [spec(arg.shape) for arg in args[scalars:]]
    return pl.pallas_call(
        kernel,
        grid=(heads,),
        in_specs=in_specs,
        out_specs=[spec(shape) for shape, _ in outs],
        out_shape=[jax.ShapeDtypeStruct(shape, dtype) for shape, dtype in outs],
        cost_estimate=pl.CostEstimate(
            flops=vmem_ops * heads, bytes_accessed=1 << 20, transcendentals=0),
        compiler_params=pltpu.CompilerParams(dimension_semantics=("arbitrary",)),
    )(*args)


def body(
    queries,
    input_key_matrix,
    input_value_matrix,
    decay_preactivation,
    extra_log_decay,
    channel_decay_speed,
    output_weight_matrix,
    stored_expert_rows,
    chosen_expert_index,
    expert_combine_weight,
    cotangent,
    expert_gate_weight,
    expert_up_weight,
    expert_down_weight,
):
    heads = input_value_matrix.shape[0] // VAL_DIM
    tok_rows = queries.shape[1]
    experts = lax.axis_size("sp")
    index = lax.axis_index("sp")
    me = index.astype(jnp.int32).reshape(1)
    capacity = 3 * tok_rows // experts
    slots = experts * capacity
    part_width = stored_expert_rows.shape[1]
    model_width = expert_gate_weight.shape[1]
    channels = heads * KEY_DIM
    values = heads * VAL_DIM
    tn = (((0,), (0,)), ((), ()))
    nt = (((1,), (1,)), ((), ()))

    expert_ids = lax.broadcasted_iota(jnp.int32, (tok_rows, experts), 1)
    picks = [chosen_expert_index[:, i:i + 1] == expert_ids for i in range(2)]
    earlier = triangle(tok_rows, lambda a, b: a > b).astype(BF16)
    counts = jnp.dot(earlier, (picks[0] | picks[1]).astype(BF16), preferred_element_type=F32)
    slot_ids = lax.broadcasted_iota(jnp.int32, (tok_rows, slots), 1)
    places = []
    for i in range(2):
        rank = jnp.sum(jnp.where(picks[i], counts, 0.0), axis=1, keepdims=True)
        slot = chosen_expert_index[:, i:i + 1] * capacity + rank.astype(jnp.int32)
        places.append((slot == slot_ids).astype(BF16))
    place = places[0] + places[1]
    weighted = [
        (expert_combine_weight[:, i:i + 1] * cotangent.astype(F32)).astype(BF16)
        for i in range(2)
    ]
    send_x = lax.dot_general(place, stored_expert_rows, tn, preferred_element_type=F32)
    send_dy = lax.dot_general(jnp.concatenate(places, axis=0), jnp.concatenate(weighted, axis=0),
                              tn, preferred_element_type=F32)

    def exchange(rows):
        rows = rows.astype(BF16).reshape(experts, capacity, part_width)
        rows = lax.all_to_all(rows, "sp", split_axis=0, concat_axis=0, tiled=True)
        return lax.all_gather(rows.reshape(slots, part_width), "tp", axis=1, tiled=True)

    rows_x = exchange(send_x)
    rows_dy = exchange(send_dy)

    speed = channel_decay_speed[:, None]
    state = ((channels, 2 * VAL_DIM), BF16)
    scores, inner, cum, fwd_sum, bwd_sum = per_head(
        head_kernel, heads,
        [((heads * tok_rows, tok_rows), BF16), ((values, tok_rows), F32),
         ((channels, tok_rows), F32), state, state],
        [queries, input_key_matrix, input_value_matrix, decay_preactivation, extra_log_decay,
         speed], 1 << 28)
    peer = lax.broadcasted_iota(jnp.int32, (experts, 1, 1), 0)
    sums = lax.all_to_all(jnp.where(peer > index, fwd_sum[None], bwd_sum[None]),
                          "sp", split_axis=0, concat_axis=0, tiled=True)
    carried, normed, inv_rms, mix_rows = per_head(
        mix_kernel, heads,
        [((channels, 2 * VAL_DIM), F32), ((values, tok_rows), F32), ((heads * 8, tok_rows), F32),
         ((values, tok_rows), BF16)],
        [me, sums, queries, cum, inner], 1 << 26, scalars=1)

    gate_local = expert_gate_weight[0]
    up_local = expert_up_weight[0]
    down_local = expert_down_weight[0]
    gate_pre = jnp.dot(rows_x, gate_local, preferred_element_type=F32)
    up_pre = jnp.dot(rows_x, up_local, preferred_element_type=F32)
    gate_sig = jax.nn.sigmoid(gate_pre)
    gate_act = gate_pre * gate_sig
    hidden = (gate_act * up_pre).astype(BF16)
    grad_hidden = lax.dot_general(rows_dy, down_local, nt, preferred_element_type=F32)
    grad_gate_pre = (grad_hidden * up_pre * gate_sig * (1.0 + gate_pre * (1.0 - gate_sig))).astype(
        BF16
    )
    grad_up_pre = (grad_hidden * gate_act).astype(BF16)
    partial_value = lax.dot_general(grad_gate_pre, gate_local, nt, preferred_element_type=F32)
    partial_value = partial_value + lax.dot_general(
        grad_up_pre, up_local, nt, preferred_element_type=F32
    )
    summed = lax.psum_scatter(
        partial_value.astype(BF16), "tp", scatter_dimension=1, tiled=True
    ).reshape(experts, capacity, part_width)
    grad_down = lax.dot_general(hidden, rows_dy, tn, preferred_element_type=F32).astype(BF16)
    grad_gate = lax.dot_general(rows_x, grad_gate_pre, tn, preferred_element_type=F32).astype(BF16)
    grad_up = lax.dot_general(rows_x, grad_up_pre, tn, preferred_element_type=F32).astype(BF16)
    returned = lax.all_to_all(summed, "sp", split_axis=0, concat_axis=0, tiled=True)
    picked = jnp.dot(place, returned.reshape(slots, part_width), preferred_element_type=F32)
    grad_rows = (cotangent.astype(F32) + picked).astype(BF16)
    full_rows = lax.all_gather(grad_rows, "tp", axis=1, tiled=True)
    grad_normed = lax.dot_general(
        output_weight_matrix, full_rows, (((0,), (1,)), ((), ())), preferred_element_type=F32
    )
    grad_out_proj = lax.psum_scatter(
        lax.dot_general(
            full_rows, mix_rows, (((0,), (1,)), ((), ())), preferred_element_type=F32
        ).astype(BF16),
        "sp",
        scatter_dimension=0,
        tiled=True,
    ).astype(F32)
    grad_mixed, fwd_source, bwd_source = per_head(
        source_kernel, heads, [((values, tok_rows), F32), state, state],
        [grad_normed, normed, inv_rms, queries, cum], 1 << 26)
    sources = lax.all_to_all(jnp.where(peer < index, fwd_source[None], bwd_source[None]),
                             "sp", split_axis=0, concat_axis=0, tiled=True)
    by_channel = ((channels, tok_rows), F32)
    grad_queries, dk, dv, dc, dt = per_head(
        inner_kernel, heads,
        [by_channel, by_channel, ((values, tok_rows), F32), by_channel, by_channel],
        [grad_mixed, queries, input_key_matrix, input_value_matrix, cum, scores, carried],
        1 << 29)
    grad_keys, grad_values, grad_logit = per_head(
        last_kernel, heads, [by_channel, ((values, tok_rows), F32), by_channel],
        [me, sources, sums, carried, input_key_matrix, input_value_matrix, cum,
         decay_preactivation, speed, dk, dv, dc, dt], 1 << 26, scalars=1)
    return (
        grad_queries,
        grad_keys,
        grad_values,
        grad_logit,
        grad_out_proj,
        grad_gate[None],
        grad_up[None],
        grad_down[None],
    )


def solution(mesh):
    in_specs = (
        P("tp", "sp"),
        P("tp", "sp"),
        P("tp", "sp"),
        P("tp", "sp"),
        P("tp", "sp"),
        P("tp"),
        P(None, "tp"),
        P("sp", "tp"),
        P("sp", None),
        P("sp", None),
        P("sp", "tp"),
        P("sp", None, "tp"),
        P("sp", None, "tp"),
        P("sp", "tp", None),
    )
    out_specs = (
        P("tp", "sp"),
        P("tp", "sp"),
        P("tp", "sp"),
        P("tp", "sp"),
        P("sp", "tp"),
        P("sp", None, "tp"),
        P("sp", None, "tp"),
        P("sp", "tp", None),
    )
    return jax.shard_map(body, mesh=mesh, in_specs=in_specs, out_specs=out_specs, check_vma=False)
```

```python
import functools

import jax
import jax.numpy as jnp
from jax import lax
from jax.experimental import pallas as pl
from jax.experimental.pallas import tpu as pltpu
from jax.sharding import PartitionSpec as P

KEY_DIM = 32
VAL_DIM = 64
BF16 = jnp.bfloat16
F32 = jnp.float32


def dot(a, b, contract):
    return lax.dot_general(a.astype(BF16), b.astype(BF16), (contract, ((), ())),
                           preferred_element_type=F32)


def exact_dot(a, b):
    return lax.dot_general(a, b, (((1,), (0,)), ((), ())), precision=lax.Precision.HIGHEST,
                           preferred_element_type=F32)


def triangle(length, test):
    rows = lax.broadcasted_iota(jnp.int32, (length, length), 0)
    cols = lax.broadcasted_iota(jnp.int32, (length, length), 1)
    return test(rows, cols)


def head_kernel(q_ref, k_ref, v_ref, pre_ref, extra_ref, speed_ref,
                st_ref, inner_ref, cum_ref, fwd_ref, bwd_ref):
    length = q_ref.shape[1]
    q = q_ref[...].astype(F32) * KEY_DIM ** (-0.5)
    k = k_ref[...].astype(F32)
    v = v_ref[...]
    pre = pre_ref[...].astype(F32)
    log_sig = jnp.minimum(pre, 0.0) - jnp.log1p(jnp.exp(-jnp.abs(pre)))
    decays = speed_ref[...] * log_sig + extra_ref[...]
    upto = triangle(length, lambda a, b: a <= b).astype(F32)
    cum = exact_dot(decays, upto)
    cum_ref[...] = cum
    cum_t = cum.T
    k_t = k.T
    total = jnp.zeros((length, length), F32)
    for c in range(KEY_DIM):
        weight = jnp.exp(-jnp.abs(cum_t[:, c:c + 1] - cum[c:c + 1, :]))
        total = total + (k_t[:, c:c + 1] * q[c:c + 1, :]) * weight
    scores = total.astype(BF16)
    st_ref[...] = scores
    inner_ref[...] = dot(v, scores, ((1,), (0,)))
    last = cum[:, length - 1:length]
    fwd = dot(k * jnp.exp(last - cum), v, ((1,), (1,)))
    bwd = dot(k * jnp.exp(cum), v, ((1,), (1,)))
    high = last.astype(BF16)
    rest = last - high.astype(F32)
    middle = rest.astype(BF16)
    low = (rest - middle.astype(F32)).astype(BF16)
    lane = lax.broadcasted_iota(jnp.int32, (KEY_DIM, VAL_DIM), 1)
    logs = jnp.where(lane == 0, high.astype(F32),
                     jnp.where(lane == 1, middle.astype(F32), low.astype(F32)))
    fwd_ref[...] = jnp.concatenate([fwd, logs], axis=1).astype(BF16)
    bwd_ref[...] = jnp.concatenate([bwd, logs], axis=1).astype(BF16)


def carry(recv, me, sums_of, factors):
    peers = recv.shape[0]
    zero = jnp.zeros((KEY_DIM, VAL_DIM), F32)
    before, after = zero, zero
    for i in range(peers):
        before = jnp.where(i < me, before * factors[i] + sums_of(i), before)
    for i in reversed(range(peers)):
        after = jnp.where(i > me, after * factors[i] + sums_of(i), after)
    return before, after


def factors_of(recv):
    out = []
    for i in range(recv.shape[0]):
        logs = recv[i, :, VAL_DIM:VAL_DIM + 3].astype(F32)
        out.append(jnp.exp(logs[:, 0:1] + logs[:, 1:2] + logs[:, 2:3]))
    return out


def mix_kernel(me_ref, recv_ref, q_ref, cum_ref, inner_ref,
               carried_ref, normed_ref, inv_ref, rows_ref):
    length = q_ref.shape[1]
    me = me_ref[0]
    fwd_in, bwd_in = carry(
        recv_ref, me, lambda i: recv_ref[i, :, :VAL_DIM].astype(F32), factors_of(recv_ref))
    carried_ref[...] = jnp.concatenate([fwd_in, bwd_in], axis=1)
    q = q_ref[...].astype(F32) * KEY_DIM ** (-0.5)
    cum = cum_ref[...]
    last = cum[:, length - 1:length]
    mixed = inner_ref[...] + dot(fwd_in, q * jnp.exp(cum), ((0,), (0,)))
    mixed = mixed + dot(bwd_in, q * jnp.exp(last - cum), ((0,), (0,)))
    inv = lax.rsqrt(jnp.mean(mixed * mixed, axis=0, keepdims=True) + 1e-06)
    normed = mixed * inv
    normed_ref[...] = normed
    inv_ref[...] = jnp.broadcast_to(inv, inv_ref.shape)
    rows_ref[...] = normed.astype(BF16)


def source_kernel(gn_ref, normed_ref, inv_ref, q_ref, cum_ref, dm_ref, fwd_ref, bwd_ref):
    length = q_ref.shape[1]
    normed = normed_ref[...]
    gn = gn_ref[...]
    dm = inv_ref[0:1, :] * (gn - normed * jnp.mean(gn * normed, axis=0, keepdims=True))
    dm_ref[...] = dm
    q = q_ref[...].astype(F32) * KEY_DIM ** (-0.5)
    cum = cum_ref[...]
    last = cum[:, length - 1:length]
    fwd = dot(q * jnp.exp(cum), dm, ((1,), (1,)))
    bwd = dot(q * jnp.exp(last - cum), dm, ((1,), (1,)))
    pad = jnp.zeros_like(fwd)
    fwd_ref[...] = jnp.concatenate([fwd, pad], axis=1).astype(BF16)
    bwd_ref[...] = jnp.concatenate([bwd, pad], axis=1).astype(BF16)


def inner_kernel(dm_ref, q_ref, k_ref, v_ref, cum_ref, st_ref, carried_ref,
                 dq_ref, dk_ref, dv_ref, dc_ref, dt_ref):
    length = q_ref.shape[1]
    dm = dm_ref[...]
    q = q_ref[...].astype(F32) * KEY_DIM ** (-0.5)
    k = k_ref[...].astype(F32)
    v = v_ref[...]
    cum = cum_ref[...]
    by_query = dot(dm, v, ((0,), (0,)))
    by_key = dot(v, dm, ((0,), (0,)))
    sign = jnp.where(triangle(length, lambda a, b: a > b), 1.0,
                     jnp.where(triangle(length, lambda a, b: a < b), -1.0, 0.0)).astype(F32)
    by_query_signed = by_query * sign
    by_key_signed = by_key * -sign
    cum_t, q_t, k_t = cum.T, q.T, k.T
    dq, dk, dq_signed, dk_signed = [], [], [], []
    for c in range(KEY_DIM):
        weight = jnp.exp(-jnp.abs(cum_t[:, c:c + 1] - cum[c:c + 1, :]))
        with_q = weight * q_t[:, c:c + 1]
        with_k = weight * k_t[:, c:c + 1]
        dk.append(jnp.sum(by_query * with_q, axis=0, keepdims=True))
        dk_signed.append(jnp.sum(by_query_signed * with_q, axis=0, keepdims=True))
        dq.append(jnp.sum(by_key * with_k, axis=0, keepdims=True))
        dq_signed.append(jnp.sum(by_key_signed * with_k, axis=0, keepdims=True))
    join = lambda rows: jnp.concatenate(rows, axis=0)
    last = cum[:, length - 1:length]
    carried = carried_ref[...]
    up, down = jnp.exp(cum), jnp.exp(last - cum)
    d_up = dot(carried[:, :VAL_DIM], dm, ((1,), (0,))) * up
    d_down = dot(carried[:, VAL_DIM:], dm, ((1,), (0,))) * down
    dq_ref[...] = (join(dq) + d_up + d_down) * KEY_DIM ** (-0.5)
    dk_ref[...] = join(dk)
    dv_ref[...] = dot(dm, st_ref[...], ((1,), (1,)))
    dc_ref[...] = q * (join(dq_signed) + d_up - d_down) - k * join(dk_signed)
    dt_ref[...] = jnp.broadcast_to(
        jnp.sum(q * d_down, axis=1, keepdims=True), dt_ref.shape)


def last_kernel(me_ref, recv_ref, first_ref, carried_ref, k_ref, v_ref, cum_ref,
                pre_ref, speed_ref, dk_in_ref, dv_in_ref, dc_in_ref, dt_ref,
                dk_ref, dv_ref, logit_ref):
    length = k_ref.shape[1]
    me = me_ref[0]
    grad_bwd, grad_fwd = carry(
        recv_ref, me, lambda i: recv_ref[i, :, :VAL_DIM].astype(F32), factors_of(first_ref))
    k = k_ref[...].astype(F32)
    v = v_ref[...]
    cum = cum_ref[...]
    last = cum[:, length - 1:length]
    up, down = jnp.exp(cum), jnp.exp(last - cum)
    d_down = dot(grad_fwd, v, ((1,), (0,))) * down
    d_up = dot(grad_bwd, v, ((1,), (0,))) * up
    dk_ref[...] = dk_in_ref[...] + d_down + d_up
    dv_ref[...] = (dv_in_ref[...] + dot(grad_fwd, k * down, ((0,), (0,)))
                   + dot(grad_bwd, k * up, ((0,), (0,))))
    carried = carried_ref[...]
    grad_factor = jnp.sum(grad_fwd * carried[:, :VAL_DIM] + grad_bwd * carried[:, VAL_DIM:],
                          axis=1, keepdims=True)
    grad_total = (dt_ref[:, 0:1] + jnp.sum(k * d_down, axis=1, keepdims=True)
                  + grad_factor * jnp.exp(last))
    dc = dc_in_ref[...] + k * (d_up - d_down)
    from_here = triangle(length, lambda a, b: a >= b).astype(F32)
    grad_decay = exact_dot(dc, from_here) + grad_total
    pre = pre_ref[...].astype(F32)
    logit_ref[...] = grad_decay * speed_ref[...] * jax.nn.sigmoid(-pre)


def per_head(kernel, heads, outs, args, vmem_ops, scalars=0):
    def spec(shape):
        if len(shape) == 3:
            return pl.BlockSpec((shape[0], shape[1] // heads, shape[2]), lambda h: (0, h, 0))
        return pl.BlockSpec((shape[0] // heads, shape[1]), lambda h: (h, 0))

    in_specs = [pl.BlockSpec(memory_space=pltpu.SMEM)] * scalars
    in_specs += [spec(arg.shape) for arg in args[scalars:]]
    return pl.pallas_call(
        kernel,
        grid=(heads,),
        in_specs=in_specs,
        out_specs=[spec(shape) for shape, _ in outs],
        out_shape=[jax.ShapeDtypeStruct(shape, dtype) for shape, dtype in outs],
        cost_estimate=pl.CostEstimate(
            flops=vmem_ops * heads, bytes_accessed=1 << 20, transcendentals=0),
        compiler_params=pltpu.CompilerParams(dimension_semantics=("arbitrary",)),
    )(*args)


def body(
    queries,
    input_key_matrix,
    input_value_matrix,
    decay_preactivation,
    extra_log_decay,
    channel_decay_speed,
    output_weight_matrix,
    stored_expert_rows,
    chosen_expert_index,
    expert_combine_weight,
    cotangent,
    expert_gate_weight,
    expert_up_weight,
    expert_down_weight,
):
    heads = input_value_matrix.shape[0] // VAL_DIM
    tok_rows = queries.shape[1]
    experts = lax.axis_size("sp")
    index = lax.axis_index("sp")
    me = index.astype(jnp.int32).reshape(1)
    capacity = 3 * tok_rows // experts
    slots = experts * capacity
    part_width = stored_expert_rows.shape[1]
    model_width = expert_gate_weight.shape[1]
    channels = heads * KEY_DIM
    values = heads * VAL_DIM
    tn = (((0,), (0,)), ((), ()))
    nt = (((1,), (1,)), ((), ()))

    expert_ids = lax.broadcasted_iota(jnp.int32, (tok_rows, experts), 1)
    picks = [chosen_expert_index[:, i:i + 1] == expert_ids for i in range(2)]
    earlier = triangle(tok_rows, lambda a, b: a > b).astype(BF16)
    counts = jnp.dot(earlier, (picks[0] | picks[1]).astype(BF16), preferred_element_type=F32)
    slot_ids = lax.broadcasted_iota(jnp.int32, (tok_rows, slots), 1)
    places = []
    for i in range(2):
        rank = jnp.sum(jnp.where(picks[i], counts, 0.0), axis=1, keepdims=True)
        slot = chosen_expert_index[:, i:i + 1] * capacity + rank.astype(jnp.int32)
        places.append((slot == slot_ids).astype(BF16))
    place = places[0] + places[1]
    weighted = [
        (expert_combine_weight[:, i:i + 1] * cotangent.astype(F32)).astype(BF16)
        for i in range(2)
    ]
    send_x = lax.dot_general(place, stored_expert_rows, tn, preferred_element_type=F32)
    send_dy = lax.dot_general(jnp.concatenate(places, axis=0), jnp.concatenate(weighted, axis=0),
                              tn, preferred_element_type=F32)

    def exchange(rows):
        rows = rows.astype(BF16).reshape(experts, capacity, part_width)
        rows = lax.all_to_all(rows, "sp", split_axis=0, concat_axis=0, tiled=True)
        return lax.all_gather(rows.reshape(slots, part_width), "tp", axis=1, tiled=True)

    rows_x = exchange(send_x)
    rows_dy = exchange(send_dy)

    speed = channel_decay_speed[:, None]
    state = ((channels, 2 * VAL_DIM), BF16)
    scores, inner, cum, fwd_sum, bwd_sum = per_head(
        head_kernel, heads,
        [((heads * tok_rows, tok_rows), BF16), ((values, tok_rows), F32),
         ((channels, tok_rows), F32), state, state],
        [queries, input_key_matrix, input_value_matrix, decay_preactivation, extra_log_decay,
         speed], 1 << 28)
    peer = lax.broadcasted_iota(jnp.int32, (experts, 1, 1), 0)
    gate_local = expert_gate_weight[0]
    up_local = expert_up_weight[0]
    gate_pre = jnp.dot(rows_x, gate_local, preferred_element_type=F32)
    up_pre = jnp.dot(rows_x, up_local, preferred_element_type=F32)
    rows_dy, fwd_sum, bwd_sum, gate_pre, up_pre = lax.optimization_barrier(
        (rows_dy, fwd_sum, bwd_sum, gate_pre, up_pre))
    sums = lax.all_to_all(jnp.where(peer > index, fwd_sum[None], bwd_sum[None]),
                          "sp", split_axis=0, concat_axis=0, tiled=True)
    carried, normed, inv_rms, mix_rows = per_head(
        mix_kernel, heads,
        [((channels, 2 * VAL_DIM), F32), ((values, tok_rows), F32), ((heads * 8, tok_rows), F32),
         ((values, tok_rows), BF16)],
        [me, sums, queries, cum, inner], 1 << 26, scalars=1)
    all_mix = lax.all_to_all(jnp.broadcast_to(mix_rows[None], (experts, values, tok_rows)),
                             "sp", split_axis=0, concat_axis=0, tiled=True)

    down_local = expert_down_weight[0]
    gate_sig = jax.nn.sigmoid(gate_pre)
    gate_act = gate_pre * gate_sig
    hidden = (gate_act * up_pre).astype(BF16)
    grad_hidden = lax.dot_general(rows_dy, down_local, nt, preferred_element_type=F32)
    grad_gate_pre = (grad_hidden * up_pre * gate_sig * (1.0 + gate_pre * (1.0 - gate_sig))).astype(
        BF16
    )
    grad_up_pre = (grad_hidden * gate_act).astype(BF16)
    partial_value = lax.dot_general(grad_gate_pre, gate_local, nt, preferred_element_type=F32)
    partial_value = partial_value + lax.dot_general(
        grad_up_pre, up_local, nt, preferred_element_type=F32
    )
    summed = lax.psum_scatter(
        partial_value.astype(BF16), "tp", scatter_dimension=1, tiled=True
    ).reshape(experts, capacity, part_width)
    grad_down = lax.dot_general(hidden, rows_dy, tn, preferred_element_type=F32).astype(BF16)
    grad_gate = lax.dot_general(rows_x, grad_gate_pre, tn, preferred_element_type=F32).astype(BF16)
    grad_up = lax.dot_general(rows_x, grad_up_pre, tn, preferred_element_type=F32).astype(BF16)
    summed, all_mix = lax.optimization_barrier((summed, all_mix))
    returned = lax.all_to_all(summed, "sp", split_axis=0, concat_axis=0, tiled=True)
    picked = jnp.dot(place, returned.reshape(slots, part_width), preferred_element_type=F32)
    grad_rows = (cotangent.astype(F32) + picked).astype(BF16)
    full_rows = lax.all_gather(grad_rows, "tp", axis=1, tiled=True)
    grad_normed = lax.dot_general(
        output_weight_matrix, full_rows, (((0,), (1,)), ((), ())), preferred_element_type=F32
    )
    grad_mixed, fwd_source, bwd_source = per_head(
        source_kernel, heads, [((values, tok_rows), F32), state, state],
        [grad_normed, normed, inv_rms, queries, cum], 1 << 26)
    sources = lax.all_to_all(jnp.where(peer < index, fwd_source[None], bwd_source[None]),
                             "sp", split_axis=0, concat_axis=0, tiled=True)
    by_channel = ((channels, tok_rows), F32)
    grad_queries, dk, dv, dc, dt = per_head(
        inner_kernel, heads,
        [by_channel, by_channel, ((values, tok_rows), F32), by_channel, by_channel],
        [grad_mixed, queries, input_key_matrix, input_value_matrix, cum, scores, carried],
        1 << 29)
    full_rows, dk = lax.optimization_barrier((full_rows, dk))
    rows_block = model_width // experts
    all_rows = lax.all_to_all(full_rows.reshape(tok_rows, experts, rows_block).swapaxes(0, 1),
                              "sp", split_axis=0, concat_axis=0, tiled=True)
    grad_out_proj = lax.dot_general(
        all_rows.reshape(experts * tok_rows, rows_block),
        all_mix.swapaxes(1, 2).reshape(experts * tok_rows, values),
        tn, preferred_element_type=F32)
    grad_keys, grad_values, grad_logit = per_head(
        last_kernel, heads, [by_channel, ((values, tok_rows), F32), by_channel],
        [me, sources, sums, carried, input_key_matrix, input_value_matrix, cum,
         decay_preactivation, speed, dk, dv, dc, dt], 1 << 26, scalars=1)
    return (
        grad_queries,
        grad_keys,
        grad_values,
        grad_logit,
        grad_out_proj,
        grad_gate[None],
        grad_up[None],
        grad_down[None],
    )


def solution(mesh):
    in_specs = (
        P("tp", "sp"),
        P("tp", "sp"),
        P("tp", "sp"),
        P("tp", "sp"),
        P("tp", "sp"),
        P("tp"),
        P(None, "tp"),
        P("sp", "tp"),
        P("sp", None),
        P("sp", None),
        P("sp", "tp"),
        P("sp", None, "tp"),
        P("sp", None, "tp"),
        P("sp", "tp", None),
    )
    out_specs = (
        P("tp", "sp"),
        P("tp", "sp"),
        P("tp", "sp"),
        P("tp", "sp"),
        P("sp", "tp"),
        P("sp", None, "tp"),
        P("sp", None, "tp"),
        P("sp", "tp", None),
    )
    return jax.shard_map(body, mesh=mesh, in_specs=in_specs, out_specs=out_specs, check_vma=False)
```
